32 devices in a mesh: sp: 16 (over z, y, core), tp: 2 (over x).
Axes of the slice: x: 2, y: 2, z: 4, core: 2. Of those that a mesh axis runs over, the one named last changes fastest.
Arguments:
- tokens: bfloat16 [8192, 2048], P(('sp', 'tp')), may hold values from -6 to 6
- norm_gain: float32 [2048], replicated, may hold values from 0.1 to 1.9
- query_weight: bfloat16 [2048, 1024], P(None, 'tp'), may hold values from -0.13258252 to 0.13258252
- key_weight: bfloat16 [2048, 1024], P(None, 'tp'), may hold values from -0.13258252 to 0.13258252
- value_weight: bfloat16 [2048, 1024], P(None, 'tp'), may hold values from -0.125 to 0.125
- glu_value_weight: bfloat16 [2048, 1024], P(None, 'tp'), may hold values from -0.125 to 0.125
- glu_gate_weight: bfloat16 [2048, 1024], P(None, 'tp'), may hold values from -0.125 to 0.125
- qk_gain: float32 [2, 64], replicated, may hold values from 1 to 6
- mix_lambda: float32 [8], P('tp'), may hold values from 0.3 to 0.8
- head_gain: float32 [128], replicated, may hold values from 0.1 to 1.9
- conv_kernel: float32 [31, 1024], P(None, 'tp'), may hold values from -1 to 1
- channel_gain: float32 [1024], P('tp'), may hold values from 0.1 to 1.9
- channel_shift: float32 [1024], P('tp'), may hold values from -3 to 3
- output_weight: bfloat16 [2048, 2048], replicated, may hold values from -0.125 to 0.125
Outputs:
- mixed: bfloat16 [8192, 2048], P(('sp', 'tp'))
- log_totals: float32 [2, 8, 8192], P(None, 'tp', 'sp')
The draws below stay inside these ranges and needn't reach their ends.
All inputs are finite; a program needn't handle non-finite values.
Results may differ from the reference program's by a relative error of at most 0.035.
Values may be sent and summed in bfloat16 or wider, within the bound.
A program may use at most 128 MiB of HBM per device.

```python
import jax
import jax.numpy as jnp
from jax import lax

D = 2048
HEADS = 8
HEAD_DIM = 64
VDIM = 128
CONV = 1024
KERNEL = 31
TOKENS = 8192
MIX = 2048


def draw_qk_gain(key, part):
    spread = jax.random.uniform(jax.random.fold_in(key, 7), (2, HEAD_DIM), jnp.float32, -1.0, 1.0)
    return 1.3 + 0.25 * spread


def paired_weights(key):
    columns = HEADS * 2 * HEAD_DIM
    factor = D ** (-0.5)
    limit = 6.0 * factor
    shared = jax.random.normal(jax.random.fold_in(key, 11), (D, columns), jnp.float32) * factor
    separate = jax.random.normal(jax.random.fold_in(key, 12), (D, columns), jnp.float32) * factor
    shared = jnp.clip(shared, -limit, limit)
    separate = jnp.clip(separate, -limit, limit)
    return (shared, separate)


def draw_query_weight(key, part):
    shared, separate = paired_weights(key)
    return shared.astype(jnp.bfloat16)


def draw_key_weight(key, part):
    shared, separate = paired_weights(key)
    return separate.astype(jnp.bfloat16)


def block_levels(rng, dims, pieces, low, largest):
    def one(position, blocks):
        draws = jax.random.uniform(jax.random.fold_in(jax.random.fold_in(rng, 6), position), (blocks,), jnp.float32, low / len(pieces), largest / len(pieces))
        return jnp.repeat(jnp.exp(draws), dims[position] // blocks).reshape((-1,) + (1,) * (len(dims) - position - 1))

    factor_of = one(*pieces[0])
    for cut in pieces[1:]:
        factor_of = factor_of * one(*cut)
    return factor_of


def normal_values(own_key, shape, width, most, split=(), held_as=jnp.bfloat16):
    drawn = width * jax.random.normal(own_key, shape, jnp.float32)
    if split:
        drawn = drawn * block_levels(own_key, shape, split, -0.22, 0.18)
    return jnp.clip(drawn, -most, most).astype(held_as)


def setup_inputs(seed: int = 0) -> dict:
    splits = jax.random.split(jax.random.key(seed), 15)
    tokens = normal_values(splits[0], (TOKENS, D), 1.0, 6.0, ((0, 32),))
    norm_gain = jnp.clip(1.0 + 0.18 * jax.random.normal(splits[1], (D,), jnp.float32), 0.1, 1.9)
    query_weight = draw_query_weight(jax.random.fold_in(splits[14], 71), 0)
    key_weight = draw_key_weight(jax.random.fold_in(splits[14], 71), 0)
    value_weight = normal_values(splits[4], (D, HEADS * VDIM), D ** -0.5, 0.125, ((1, 2),))
    glu_value_weight = normal_values(splits[5], (D, CONV), D ** -0.5, 0.125, ((1, 2),))
    glu_gate_weight = normal_values(splits[6], (D, CONV), D ** -0.5, 0.125, ((1, 2),))
    qk_gain = draw_qk_gain(jax.random.fold_in(splits[14], 71), 0)
    mix_lambda = jnp.clip(0.3 + 0.5 * jax.random.uniform(splits[8], (HEADS,), jnp.float32) ** block_levels(splits[8], (HEADS,), ((0, 2),), -0.2, 0.2), 0.3, 0.8)
    head_gain = jnp.clip(1.0 + 0.18 * jax.random.normal(splits[9], (VDIM,), jnp.float32), 0.1, 1.9)
    conv_kernel = normal_values(splits[10], (KERNEL, CONV), KERNEL ** -0.5, 1.0, ((1, 2),), jnp.float32)
    channel_gain = jnp.clip(1.0 + 0.18 * jax.random.normal(splits[11], (CONV,), jnp.float32), 0.1, 1.9)
    channel_shift = normal_values(splits[12], (CONV,), 0.5, 3.0, ((0, 2),), jnp.float32)
    output_weight = normal_values(splits[13], (MIX, D), MIX ** -0.5, 0.125)
    return dict(tokens=tokens, norm_gain=norm_gain, query_weight=query_weight, key_weight=key_weight, value_weight=value_weight, glu_value_weight=glu_value_weight, glu_gate_weight=glu_gate_weight, qk_gain=qk_gain, mix_lambda=mix_lambda, head_gain=head_gain, conv_kernel=conv_kernel, channel_gain=channel_gain, channel_shift=channel_shift, output_weight=output_weight)


def rotate(values, positions):
    half = values.shape[-1] // 2
    inverse = 10000.0 ** (-jnp.arange(0, half, dtype=jnp.float32) * 2.0 / values.shape[-1])
    angles = positions[:, None] * inverse[None, :]
    cosine = jnp.cos(angles)[:, None, None, :]
    sine = jnp.sin(angles)[:, None, None, :]
    first = values[..., :half]
    second = values[..., half:]
    return jnp.concatenate([first * cosine - second * sine, second * cosine + first * sine], axis=-1)

def prepare(raw, qk_gain, positions):
    values = raw.astype(jnp.float32)
    values = values * lax.rsqrt(lax.optimization_barrier(jnp.mean(values * values, axis=-1, keepdims=True)) + 1e-06)
    values = values * qk_gain[None, None, :, :]
    return rotate(values, positions).astype(jnp.bfloat16)

def reference(tokens, norm_gain, query_weight, key_weight, value_weight, glu_value_weight, glu_gate_weight, qk_gain, mix_lambda, head_gain, conv_kernel, channel_gain, channel_shift, output_weight):
    inputs = tokens.astype(jnp.float32)
    normed = (inputs * lax.rsqrt(lax.optimization_barrier(jnp.mean(inputs * inputs, axis=-1, keepdims=True)) + 1e-06) * norm_gain).astype(jnp.bfloat16)
    queries = jnp.dot(normed, query_weight, preferred_element_type=jnp.float32).astype(jnp.bfloat16).reshape(TOKENS, HEADS, 2, HEAD_DIM)
    keys = jnp.dot(normed, key_weight, preferred_element_type=jnp.float32).astype(jnp.bfloat16).reshape(TOKENS, HEADS, 2, HEAD_DIM)
    values = jnp.dot(normed, value_weight, preferred_element_type=jnp.float32).astype(jnp.bfloat16).reshape(TOKENS, HEADS, VDIM)
    glu_a = jnp.dot(normed, glu_value_weight, preferred_element_type=jnp.float32).astype(jnp.bfloat16)
    glu_g = jnp.dot(normed, glu_gate_weight, preferred_element_type=jnp.float32).astype(jnp.bfloat16)
    positions = jnp.arange(TOKENS, dtype=jnp.int32)
    rq = prepare(queries, qk_gain, positions.astype(jnp.float32))
    rk = prepare(keys, qk_gain, positions.astype(jnp.float32))
    key_heads = jnp.transpose(rk, (1, 0, 2, 3)).astype(jnp.float32)
    value_heads = jnp.transpose(values, (1, 0, 2)).astype(jnp.float32)
    block = 512
    blocks = TOKENS // block
    query_blocks = rq.reshape(blocks, block, HEADS, 2, HEAD_DIM)
    starts = jnp.arange(blocks, dtype=jnp.int32) * block
    scale = HEAD_DIM ** (-0.5)

    def one_block(item):
        query_block, begin = item
        query_pos = begin + jnp.arange(block, dtype=jnp.int32)
        allowed = positions[None, :] <= query_pos[:, None]

        def one_head(head_item):
            query_head, key_head, value_head, weight_two = head_item
            scores = jnp.einsum('qmd,kmd->mqk', query_head.astype(jnp.float32), key_head) * scale
            scores = jnp.where(allowed[None], scores, -1e+30)
            top = lax.optimization_barrier(jnp.max(scores, axis=-1))
            probs = jnp.where(allowed[None], jnp.exp(scores - top[..., None]), 0.0)
            total = lax.optimization_barrier(jnp.sum(probs, axis=-1))
            rounded = probs.astype(jnp.bfloat16).astype(jnp.float32)
            summed = jnp.einsum('mqk,kd->mqd', rounded, value_head)
            heads_out = summed[0] / total[0][:, None] - weight_two * summed[1] / total[1][:, None]
            heads_out = heads_out * lax.rsqrt(lax.optimization_barrier(jnp.mean(heads_out * heads_out, axis=-1, keepdims=True)) + 1e-06) * head_gain
            return (heads_out.astype(jnp.bfloat16), top + jnp.log(total))
        return lax.map(one_head, (jnp.transpose(query_block, (1, 0, 2, 3)), key_heads, value_heads, mix_lambda))
    outputs, totals = lax.map(one_block, (query_blocks, starts))
    attended = jnp.transpose(outputs, (0, 2, 1, 3)).reshape(TOKENS, HEADS * VDIM)
    log_totals = jnp.transpose(totals, (2, 1, 0, 3)).reshape(2, HEADS, TOKENS)
    gated = (glu_a.astype(jnp.float32) * jax.nn.sigmoid(glu_g.astype(jnp.float32))).astype(jnp.bfloat16)
    padded = jnp.concatenate([jnp.zeros((KERNEL - 1, CONV), jnp.float32), gated.astype(jnp.float32)], axis=0)
    convolved = jnp.zeros((TOKENS, CONV), jnp.float32)
    for offset in range(KERNEL):
        convolved = convolved + conv_kernel[offset][None, :] * padded[offset:offset + TOKENS]
    middle = lax.optimization_barrier(jnp.mean(convolved, axis=-1, keepdims=True))
    spread = lax.optimization_barrier(jnp.mean(convolved * convolved, axis=-1, keepdims=True)) - middle * middle
    conv_out = jax.nn.silu((convolved - middle) * lax.rsqrt(spread + 1e-05) * channel_gain + channel_shift).astype(jnp.bfloat16)
    merged = jnp.concatenate([attended, conv_out], axis=1)
    mixed = jnp.dot(merged, output_weight, preferred_element_type=jnp.float32).astype(jnp.bfloat16)
    return (mixed, log_totals)
```

```python
import math

import jax
import jax.numpy as jnp
from jax import lax
from jax.experimental import pallas as pl
from jax.experimental.pallas import tpu as pltpu
from jax.sharding import PartitionSpec as P

MESH = pl.DeviceIdType.MESH
NEG = -1e30


def from_behind(value, axis, steps):
    count = lax.axis_size(axis)
    leading, last = (max(0, -steps), min(count, count - steps))
    return lax.ppermute(value, axis, [(source, source + steps) for source in range(leading, last)])


def spread_kernel(ways, group, q_ref, kv_ref, qo_ref, kvo_ref, qsend, qrecv, ksend, kfwd, krelay, krecv, local):
    me = lax.axis_index("sp")
    a = me // group
    g = me % group
    cores = 2 if group % 2 == 0 else 1
    half = group // cores
    mate = a * group + (g + 1 - 2 * (g % 2)) if cores == 2 else me

    def same(d):
        return (g + d * cores) % group

    peers = [lax.rem(a + d, ways) * group + g for d in range(1, ways)]
    peers += [a * group + same(d) for d in range(1, half)]
    if cores == 2:
        peers.append(mate)
    barrier = pltpu.get_barrier_semaphore()
    for peer in peers:
        pl.semaphore_signal(barrier, inc=1, device_id={"sp": peer}, device_id_type=MESH)
    pl.semaphore_wait(barrier, len(peers))

    def kv_copy(src, slot, send, peer):
        return pltpu.make_async_remote_copy(
            src_ref=src, dst_ref=kvo_ref.at[slot], send_sem=send, recv_sem=krecv.at[slot],
            device_id={"sp": peer}, device_id_type=MESH)

    sends = []
    locals_ = [
        pltpu.make_async_copy(kv_ref.at[a], kvo_ref.at[me], local.at[0]),
        pltpu.make_async_copy(q_ref.at[a], qo_ref.at[a], local.at[1]),
    ]
    for c in locals_:
        c.start()
    order = list(range(1, ways))
    for d in order:
        h = lax.rem(a + d, ways)
        c = kv_copy(kv_ref.at[h], me, ksend.at[d - 1], h * group + g)
        c.start()
        sends.append(c)

    def forward(d):
        src_a = lax.rem(a + ways - d, ways)
        slot = src_a * group + g
        if d:
            kv_copy(kvo_ref.at[slot], slot, ksend.at[d - 1], me).wait_recv()
            src = kvo_ref.at[slot]
        else:
            src = kv_ref.at[a]
        n = 0
        for e in range(1, half):
            c = kv_copy(src, slot, kfwd.at[d, n], a * group + same(e))
            c.start()
            sends.append(c)
            n += 1
        if cores == 2:
            c = kv_copy(src, slot, kfwd.at[d, n], mate)
            c.start()
            sends.append(c)

    def relay(d):
        src_a = lax.rem(a + ways - d, ways)
        for e in range(1, half):
            slot = src_a * group + same(e)
            kv_copy(kvo_ref.at[slot], slot, krelay.at[d, e - 1], mate).wait_recv()
            if cores == 2:
                c = kv_copy(kvo_ref.at[slot], slot, krelay.at[d, e - 1], mate)
                c.start()
                sends.append(c)

    forward(0)
    for d in order:
        h = lax.rem(a + d, ways)
        c = pltpu.make_async_remote_copy(
            src_ref=q_ref.at[h], dst_ref=qo_ref.at[a], send_sem=qsend.at[d - 1], recv_sem=qrecv.at[a],
            device_id={"sp": h * group + g}, device_id_type=MESH)
        c.start()
        sends.append(c)
    for d in range(1, ways):
        forward(d)
        relay(d - 1)
    relay(ways - 1)
    if cores == 2:
        for d in range(ways):
            src_a = lax.rem(a + ways - d, ways)
            for e in range(half):
                slot = src_a * group + (g + 1 - 2 * (g % 2) + e * cores) % group
                kv_copy(kvo_ref.at[slot], slot, krelay.at[0, 0], mate).wait_recv()
    for d in range(1, ways):
        src_a = lax.rem(a + ways - d, ways)
        pltpu.make_async_remote_copy(
            src_ref=q_ref.at[a], dst_ref=qo_ref.at[src_a], send_sem=qsend.at[d - 1],
            recv_sem=qrecv.at[src_a], device_id={"sp": me}, device_id_type=MESH).wait_recv()
    for c in sends:
        c.wait_send()
    for c in locals_:
        c.wait()


def spread(q, kv, ways, group):
    cores = 2 if group % 2 == 0 else 1
    half = group // cores
    any_ = pl.BlockSpec(memory_space=pl.ANY)
    n = max(ways - 1, 1)
    return pl.pallas_call(
        lambda *refs: spread_kernel(ways, group, *refs),
        out_shape=(
            jax.ShapeDtypeStruct(q.shape, q.dtype),
            jax.ShapeDtypeStruct((ways * group,) + kv.shape[1:], kv.dtype),
        ),
        in_specs=[any_, any_],
        out_specs=(any_, any_),
        scratch_shapes=[
            pltpu.SemaphoreType.DMA((n,)),
            pltpu.SemaphoreType.DMA((ways,)),
            pltpu.SemaphoreType.DMA((n,)),
            pltpu.SemaphoreType.DMA((ways, half)),
            pltpu.SemaphoreType.DMA((ways, max(half - 1, 1))),
            pltpu.SemaphoreType.DMA((ways * group,)),
            pltpu.SemaphoreType.DMA((2,)),
        ],
        compiler_params=pltpu.CompilerParams(collective_id=1, has_side_effects=True),
        name="spread",
    )(q, kv)


def collect_kernel(ways, group, tp, att_ref, lt_ref, conv_ref, ao_ref, lo_ref, co_ref, asend, arecv, lsend, lrecv, csend, crecv, local):
    me = lax.axis_index("sp")
    t = lax.axis_index("tp")
    a = me // group
    g = me % group
    vdim = att_ref.shape[-1]
    cch = conv_ref.shape[-1]

    def coords(i):
        dt, da = i % tp, i // tp
        return lax.rem(a + da, ways), lax.rem(t + dt, tp)

    total = ways * tp
    barrier = pltpu.get_barrier_semaphore()
    for i in range(1, total):
        pa, pt = coords(i)
        pl.semaphore_signal(barrier, inc=1, device_id={"sp": pa * group + g, "tp": pt}, device_id_type=MESH)
    pl.semaphore_wait(barrier, total - 1)

    head = t * ways + a
    sends = []
    for i in list(range(total - 1, 0, -1)):
        pa, pt = coords(i)
        dev = {"sp": pa * group + g, "tp": pt}
        c = pltpu.make_async_remote_copy(
            src_ref=att_ref.at[pa, pt], dst_ref=ao_ref.at[head],
            send_sem=asend.at[i], recv_sem=arecv.at[head], device_id=dev, device_id_type=MESH)
        c.start()
        sends.append(c)
    for i in range(1, tp):
        pa, pt = coords(i)
        c = pltpu.make_async_remote_copy(
            src_ref=conv_ref.at[pt], dst_ref=co_ref.at[t],
            send_sem=csend.at[i], recv_sem=crecv.at[t],
            device_id={"sp": me, "tp": pt}, device_id_type=MESH)
        c.start()
        sends.append(c)
    for i in range(1, ways):
        pa = lax.rem(a + i, ways)
        c = pltpu.make_async_remote_copy(
            src_ref=lt_ref.at[pa], dst_ref=lo_ref.at[a], send_sem=lsend.at[i], recv_sem=lrecv.at[a],
            device_id={"sp": pa * group + g, "tp": t}, device_id_type=MESH)
        c.start()
        sends.append(c)
    mine = [
        pltpu.make_async_copy(att_ref.at[a, t], ao_ref.at[head], local.at[0]),
        pltpu.make_async_copy(conv_ref.at[t], co_ref.at[t], local.at[1]),
        pltpu.make_async_copy(lt_ref.at[a], lo_ref.at[a], local.at[2]),
    ]
    for c in mine:
        c.start()
    for i in range(1, total):
        pa, pt = coords(i)
        h = pt * ways + pa
        pltpu.make_async_remote_copy(
            src_ref=att_ref.at[a, t], dst_ref=ao_ref.at[h],
            send_sem=asend.at[i], recv_sem=arecv.at[h],
            device_id={"sp": me, "tp": t}, device_id_type=MESH).wait_recv()
    for i in range(1, tp):
        pa, pt = coords(i)
        pltpu.make_async_remote_copy(
            src_ref=conv_ref.at[t], dst_ref=co_ref.at[pt],
            send_sem=csend.at[i], recv_sem=crecv.at[pt],
            device_id={"sp": me, "tp": t}, device_id_type=MESH).wait_recv()
    for i in range(1, ways):
        pa = lax.rem(a + i, ways)
        pltpu.make_async_remote_copy(
            src_ref=lt_ref.at[a], dst_ref=lo_ref.at[pa], send_sem=lsend.at[i], recv_sem=lrecv.at[pa],
            device_id={"sp": me, "tp": t}, device_id_type=MESH).wait_recv()
    for c in sends:
        c.wait_send()
    for c in mine:
        c.wait()


def collect(att, lt, conv, ways, group, tp):
    any_ = pl.BlockSpec(memory_space=pl.ANY)
    rows, vdim = att.shape[2:]
    total = ways * tp
    return pl.pallas_call(
        lambda *refs: collect_kernel(ways, group, tp, *refs),
        out_shape=(
            jax.ShapeDtypeStruct((total, rows, vdim), att.dtype),
            jax.ShapeDtypeStruct(lt.shape, lt.dtype),
            jax.ShapeDtypeStruct(conv.shape, conv.dtype),
        ),
        in_specs=[any_] * 3,
        out_specs=(any_,) * 3,
        scratch_shapes=[
            pltpu.SemaphoreType.DMA((total,)),
            pltpu.SemaphoreType.DMA((total,)),
            pltpu.SemaphoreType.DMA((ways,)),
            pltpu.SemaphoreType.DMA((ways,)),
            pltpu.SemaphoreType.DMA((tp,)),
            pltpu.SemaphoreType.DMA((tp,)),
            pltpu.SemaphoreType.DMA((3,)),
        ],
        compiler_params=pltpu.CompilerParams(collective_id=2, has_side_effects=True),
        name="collect",
    )(att, lt, conv)


def attention(place, lam, head_gain, qt, kv, tile=512):
    ways, qdim, rows = qt.shape
    hd = qdim // 2
    blocks = kv.shape[0]
    vdim = head_gain.shape[0]
    group = blocks // ways
    tile = min(tile, rows)
    tiles = rows // tile

    def kernel(place_ref, lam_ref, gain_ref, q_ref, kv_ref, o_ref, lt_ref):
        i = pl.program_id(0)
        s = pl.program_id(1)
        chunk = i * group + place_ref[0]
        qs = [q_ref[0, m * hd:(m + 1) * hd, :] for m in range(2)]

        def step(j, carry, masked):
            out = []
            kb = kv_ref[j, :rows]
            vb = jnp.concatenate(
                [kv_ref[j, rows + b * vdim:rows + (b + 1) * vdim] for b in range(rows // 128)], axis=1)
            for m in range(2):
                top, tot, acc = carry[m]
                sc = jnp.dot(kb[:, m * hd:(m + 1) * hd], qs[m], preferred_element_type=jnp.float32)
                if masked:
                    kp = lax.broadcasted_iota(jnp.int32, sc.shape, 0)
                    qp = lax.broadcasted_iota(jnp.int32, sc.shape, 1) + s * tile
                    sc = jnp.where(kp <= qp, sc, NEG)
                new = jnp.maximum(top, jnp.max(sc, axis=0, keepdims=True))
                p = jnp.exp(sc - new)
                f = jnp.exp(top - new)
                tot = tot * f + jnp.sum(p, axis=0, keepdims=True)
                acc = acc * f + jnp.dot(vb, p.astype(jnp.bfloat16), preferred_element_type=jnp.float32)
                out.append((new, tot, acc))
            return tuple(out)

        one = (jnp.full((1, tile), NEG, jnp.float32), jnp.zeros((1, tile), jnp.float32),
               jnp.zeros((vdim, tile), jnp.float32))
        carry = step(chunk, (one, one), True)
        carry = lax.fori_loop(0, chunk, lambda j, c: step(j, c, False), carry)
        (t0, l0, a0), (t1, l1, a1) = carry
        heads = a0 / l0 - lam_ref[0] * a1 / l1
        heads = heads * lax.rsqrt(jnp.mean(heads * heads, axis=0, keepdims=True) + 1e-06) * gain_ref[...]
        o_ref[0] = heads.T.astype(jnp.bfloat16)
        lt_ref[0, 0:1, :] = t0 + jnp.log(l0)
        lt_ref[0, 1:2, :] = t1 + jnp.log(l1)

    smem = pl.BlockSpec(memory_space=pltpu.SMEM)
    return pl.pallas_call(
        kernel,
        grid=(ways, tiles),
        out_shape=(
            jax.ShapeDtypeStruct((ways, rows, vdim), jnp.bfloat16),
            jax.ShapeDtypeStruct((ways, 2, rows), jnp.float32),
        ),
        in_specs=[
            smem, smem,
            pl.BlockSpec((vdim, 1), lambda i, s: (0, 0)),
            pl.BlockSpec((1, qdim, tile), lambda i, s: (i, 0, s)),
            pl.BlockSpec(kv.shape, lambda i, s: (0, 0, 0)),
        ],
        out_specs=(
            pl.BlockSpec((1, tile, vdim), lambda i, s: (i, s, 0)),
            pl.BlockSpec((1, 2, tile), lambda i, s: (i, 0, s)),
        ),
        compiler_params=pltpu.CompilerParams(vmem_limit_bytes=50 << 20),
        name="attend",
    )(place, lam, head_gain.reshape(-1, 1), qt, kv)


def prepare_t(raw, qk_gain, cosine, sine):
    values = raw.astype(jnp.float32)
    values = values * lax.rsqrt(jnp.mean(values * values, axis=2, keepdims=True) + 1e-06)
    values = values * qk_gain[None, :, :, None]
    half = raw.shape[2] // 2
    first, second = values[:, :, :half], values[:, :, half:]
    return jnp.concatenate(
        [first * cosine - second * sine, second * cosine + first * sine], axis=2
    ).astype(jnp.bfloat16)


def per_device(
    tokens, norm_gain, query_weight, key_weight, value_weight, glu_value_weight, glu_gate_weight,
    qk_gain, mix_lambda, head_gain, conv_kernel, channel_gain, channel_shift, output_weight,
):
    head_size = qk_gain.shape[1]
    heads_here = mix_lambda.shape[0]
    value_size = head_gain.shape[0]
    kernel_len = conv_kernel.shape[0]
    conv_here = conv_kernel.shape[1]
    width = tokens.shape[1]
    sp = lax.axis_size("sp")
    tp = lax.axis_size("tp")
    me = lax.axis_index("sp")
    t = lax.axis_index("tp")
    ways = heads_here
    group = sp // ways
    own = tokens.shape[0]
    rows = own * tp

    def norm(piece):
        inputs = piece.astype(jnp.float32)
        return (
            inputs * lax.rsqrt(jnp.mean(inputs * inputs, axis=-1, keepdims=True) + 1e-06) * norm_gain
        ).astype(jnp.bfloat16)

    others = [tokens] + [
        lax.ppermute(tokens, "tp", [(i, (i - d) % tp) for i in range(tp)]) for d in range(1, tp)
    ]
    if tp == 2:
        other = others[1]
        normed = norm(jnp.concatenate([jnp.where(t == 0, tokens, other), jnp.where(t == 0, other, tokens)], axis=0))
    else:
        stacked = jnp.stack(others)
        normed = norm(jnp.concatenate(
            [lax.dynamic_index_in_dim(stacked, (j - t) % tp, 0, keepdims=False) for j in range(tp)], axis=0))

    def turned(matrix):
        return lax.dot_general(matrix, normed, (((0,), (1,)), ((), ())), preferred_element_type=jnp.float32).astype(jnp.bfloat16)

    def plain(matrix):
        return jnp.dot(normed, matrix, preferred_element_type=jnp.float32).astype(jnp.bfloat16)

    positions = (me * rows + jnp.arange(rows, dtype=jnp.int32)).astype(jnp.float32)
    inverse = 10000.0 ** (-jnp.arange(0, head_size // 2, dtype=jnp.float32) * 2.0 / head_size)
    angles = positions[None, :] * inverse[:, None]
    cosine, sine = jnp.cos(angles)[None, None], jnp.sin(angles)[None, None]
    shape = (heads_here, 2, head_size, rows)
    rq = prepare_t(turned(query_weight).reshape(shape), qk_gain, cosine, sine) * jnp.bfloat16(head_size ** -0.5)
    rk = prepare_t(turned(key_weight).reshape(shape), qk_gain, cosine, sine)
    qt = rq.reshape(heads_here, 2 * head_size, rows)
    kk = jnp.transpose(rk.reshape(heads_here, 2 * head_size, rows), (0, 2, 1))
    vt = turned(value_weight).reshape(heads_here, value_size, rows)
    kv = jnp.concatenate([kk, vt.reshape(heads_here, value_size, rows // 128, 128).transpose(0, 2, 1, 3).reshape(heads_here, -1, 128)], axis=1)
    qall, kvall = spread(qt, kv, ways, group)

    glu_a, glu_g = plain(glu_value_weight), plain(glu_gate_weight)
    gated = (glu_a.astype(jnp.float32) * jax.nn.sigmoid(glu_g.astype(jnp.float32))).astype(jnp.bfloat16)
    earlier = from_behind(gated[rows - (kernel_len - 1):], "sp", 1)
    extended = jnp.concatenate([earlier, gated], axis=0).astype(jnp.float32)
    convolved = jnp.zeros((rows, conv_here), jnp.float32)
    for step in range(kernel_len):
        convolved = convolved + conv_kernel[step][None, :] * extended[step:step + rows]
    plain_sum, square_sum = lax.psum(
        (jnp.sum(convolved, axis=1), jnp.sum(convolved * convolved, axis=1)), "tp"
    )
    channels = conv_here * tp
    middle = (plain_sum / channels)[:, None]
    spread_ = (square_sum / channels)[:, None] - middle * middle
    conv_out = jax.nn.silu(
        (convolved - middle) * lax.rsqrt(spread_ + 1e-05) * channel_gain + channel_shift
    ).astype(jnp.bfloat16)

    place = (me % group).astype(jnp.int32).reshape(1)
    lam = lax.dynamic_slice(mix_lambda, (me // group,), (1,))
    att, lt = attention(place, lam, head_gain, qall, kvall)
    ao, lo, co = collect(
        att.reshape(ways, tp, own, value_size), lt, conv_out.reshape(tp, own, conv_here), ways, group, tp)
    heads = ways * tp
    merged = jnp.concatenate([
        jnp.transpose(ao, (1, 0, 2)).reshape(own, heads * value_size),
        jnp.transpose(co, (1, 0, 2)).reshape(own, channels)], axis=1)
    mixed = jnp.dot(merged, output_weight, preferred_element_type=jnp.float32).astype(jnp.bfloat16)
    return (mixed, jnp.transpose(lo, (1, 0, 2)))


def solution(mesh):
    placed = (
        P(("sp", "tp"), None), P(), P(None, "tp"), P(None, "tp"), P(None, "tp"), P(None, "tp"), P(None, "tp"),
        P(), P("tp"), P(), P(None, "tp"), P("tp"), P("tp"), P(),
    )
    return jax.shard_map(
        per_device,
        mesh=mesh,
        in_specs=placed,
        out_specs=(P(("sp", "tp"), None), P(None, "tp", "sp")),
        check_vma=False,
    )
```

```python
import math

import jax
import jax.numpy as jnp
from jax import lax
from jax.experimental import pallas as pl
from jax.experimental.pallas import tpu as pltpu
from jax.sharding import PartitionSpec as P

MESH = pl.DeviceIdType.MESH
NEG = -1e30


def from_behind(value, axis, steps):
    count = lax.axis_size(axis)
    leading, last = (max(0, -steps), min(count, count - steps))
    return lax.ppermute(value, axis, [(source, source + steps) for source in range(leading, last)])


def flipped(g, a, group):
    if group % 2:
        return g
    return jnp.where(a % 2 == 0, g, group - 1 - g)


def spread_kernel(ways, group, q_ref, kv_ref, qo_ref, kvo_ref, qsend, qrecv, ksend, kfwd, krelay, krecv, local):
    me = lax.axis_index("sp")
    a = me // group
    g = me % group
    cores = 2 if group % 2 == 0 else 1
    half = group // cores
    mate = a * group + (g + 1 - 2 * (g % 2)) if cores == 2 else me

    def same(d):
        return (g + d * cores) % group

    peers = [lax.rem(a + d, ways) * group + g for d in range(1, ways)]
    peers += [a * group + same(d) for d in range(1, half)]
    if cores == 2:
        peers.append(mate)
        peers += [lax.rem(a + d, ways) * group + group - 1 - g for d in range(ways)]
    barrier = pltpu.get_barrier_semaphore()
    for peer in peers:
        pl.semaphore_signal(barrier, inc=1, device_id={"sp": peer}, device_id_type=MESH)
    pl.semaphore_wait(barrier, len(peers))

    def kv_copy(src, slot, send, peer):
        return pltpu.make_async_remote_copy(
            src_ref=src, dst_ref=kvo_ref.at[slot], send_sem=send, recv_sem=krecv.at[slot],
            device_id={"sp": peer}, device_id_type=MESH)

    sends = []
    keep = pltpu.make_async_copy(kv_ref.at[a], kvo_ref.at[me], local.at[0])
    keep_q = pltpu.make_async_copy(q_ref.at[a], qo_ref.at[a], local.at[1])
    keep.start()

    def q_copy(h, slot, d):
        return pltpu.make_async_remote_copy(
            src_ref=q_ref.at[h], dst_ref=qo_ref.at[slot], send_sem=qsend.at[d], recv_sem=qrecv.at[slot],
            device_id={"sp": h * group + flipped(g, a, group)}, device_id_type=MESH)

    stays = a % 2 == 0 if cores == 2 else a >= 0

    @pl.when(stays)
    def _():
        keep_q.start()
    order = list(range(1, ways))
    for d in order:
        h = lax.rem(a + d, ways)
        c = kv_copy(kv_ref.at[h], me, ksend.at[d - 1], h * group + g)
        c.start()
        sends.append(c)

    def forward(d):
        src_a = lax.rem(a + ways - d, ways)
        slot = src_a * group + g
        if d:
            kv_copy(kvo_ref.at[slot], slot, ksend.at[d - 1], me).wait_recv()
            src = kvo_ref.at[slot]
        else:
            src = kv_ref.at[a]
        n = 0
        for e in range(1, half):
            c = kv_copy(src, slot, kfwd.at[d, n], a * group + same(e))
            c.start()
            sends.append(c)
            n += 1
        if cores == 2:
            c = kv_copy(src, slot, kfwd.at[d, n], mate)
            c.start()
            sends.append(c)

    def relay(d):
        src_a = lax.rem(a + ways - d, ways)
        for e in range(1, half):
            slot = src_a * group + same(e)
            kv_copy(kvo_ref.at[slot], slot, krelay.at[d, e - 1], mate).wait_recv()
            if cores == 2:
                c = kv_copy(kvo_ref.at[slot], slot, krelay.at[d, e - 1], mate)
                c.start()
                sends.append(c)

    forward(0)
    for d in order:
        c = q_copy(lax.rem(a + d, ways), a, d)
        c.start()
        sends.append(c)
    if cores == 2:
        @pl.when(jnp.logical_not(stays))
        def _():
            q_copy(a, a, 0).start()
    for d in range(1, ways):
        forward(d)
        relay(d - 1)
    relay(ways - 1)
    if cores == 2:
        for d in range(ways):
            src_a = lax.rem(a + ways - d, ways)
            for e in range(half):
                slot = src_a * group + (g + 1 - 2 * (g % 2) + e * cores) % group
                kv_copy(kvo_ref.at[slot], slot, krelay.at[0, 0], mate).wait_recv()
    for d in range(1, ways):
        src_a = lax.rem(a + ways - d, ways)
        q_copy(a, src_a, d).wait_recv()
    for c in sends:
        c.wait_send()
    keep.wait()

    @pl.when(stays)
    def _():
        keep_q.wait()

    if cores == 2:
        @pl.when(jnp.logical_not(stays))
        def _():
            q_copy(a, a, 0).wait()


def spread(q, kv, ways, group):
    cores = 2 if group % 2 == 0 else 1
    half = group // cores
    any_ = pl.BlockSpec(memory_space=pl.ANY)
    n = max(ways - 1, 1)
    return pl.pallas_call(
        lambda *refs: spread_kernel(ways, group, *refs),
        out_shape=(
            jax.ShapeDtypeStruct(q.shape, q.dtype),
            jax.ShapeDtypeStruct((ways * group,) + kv.shape[1:], kv.dtype),
        ),
        in_specs=[any_, any_],
        out_specs=(any_, any_),
        scratch_shapes=[
            pltpu.SemaphoreType.DMA((ways,)),
            pltpu.SemaphoreType.DMA((ways,)),
            pltpu.SemaphoreType.DMA((n,)),
            pltpu.SemaphoreType.DMA((ways, half)),
            pltpu.SemaphoreType.DMA((ways, max(half - 1, 1))),
            pltpu.SemaphoreType.DMA((ways * group,)),
            pltpu.SemaphoreType.DMA((2,)),
        ],
        compiler_params=pltpu.CompilerParams(collective_id=1, has_side_effects=True),
        name="spread",
    )(q, kv)


def collect_kernel(ways, group, tp, att_ref, lt_ref, conv_ref, ao_ref, lo_ref, co_ref, asend, arecv, lsend, lrecv, csend, crecv, local):
    me = lax.axis_index("sp")
    t = lax.axis_index("tp")
    a = me // group
    g = me % group
    vdim = att_ref.shape[-1]
    cch = conv_ref.shape[-1]

    def coords(i):
        dt, da = i % tp, i // tp
        return lax.rem(a + da, ways), lax.rem(t + dt, tp)

    total = ways * tp
    both = group % 2 == 0
    barrier = pltpu.get_barrier_semaphore()
    for i in range(total):
        pa, pt = coords(i)
        if i:
            pl.semaphore_signal(barrier, inc=1, device_id={"sp": pa * group + g, "tp": pt}, device_id_type=MESH)
        if both:
            pl.semaphore_signal(
                barrier, inc=1, device_id={"sp": pa * group + group - 1 - g, "tp": pt}, device_id_type=MESH)
    pl.semaphore_wait(barrier, 2 * total - 1 if both else total - 1)

    head = t * ways + a

    def att_copy(i, slot):
        pa, pt = coords(i)
        return pltpu.make_async_remote_copy(
            src_ref=att_ref.at[pa, pt], dst_ref=ao_ref.at[slot], send_sem=asend.at[i], recv_sem=arecv.at[slot],
            device_id={"sp": pa * group + flipped(g, pa, group), "tp": pt}, device_id_type=MESH)

    def lt_copy(i, slot):
        pa = lax.rem(a + i, ways)
        return pltpu.make_async_remote_copy(
            src_ref=lt_ref.at[pa], dst_ref=lo_ref.at[slot], send_sem=lsend.at[i], recv_sem=lrecv.at[slot],
            device_id={"sp": pa * group + flipped(g, pa, group), "tp": t}, device_id_type=MESH)

    stays = a % 2 == 0 if both else a >= 0
    sends = []
    for i in range(total - 1, 0, -1):
        c = att_copy(i, head)
        c.start()
        sends.append(c)
    for i in range(1, tp):
        pa, pt = coords(i)
        c = pltpu.make_async_remote_copy(
            src_ref=conv_ref.at[pt], dst_ref=co_ref.at[t],
            send_sem=csend.at[i], recv_sem=crecv.at[t],
            device_id={"sp": me, "tp": pt}, device_id_type=MESH)
        c.start()
        sends.append(c)
    for i in range(1, ways):
        c = lt_copy(i, a)
        c.start()
        sends.append(c)
    keep = pltpu.make_async_copy(conv_ref.at[t], co_ref.at[t], local.at[1])
    keep.start()
    mine = [
        pltpu.make_async_copy(att_ref.at[a, t], ao_ref.at[head], local.at[0]),
        pltpu.make_async_copy(lt_ref.at[a], lo_ref.at[a], local.at[2]),
    ]

    @pl.when(stays)
    def _():
        for c in mine:
            c.start()

    if both:
        @pl.when(jnp.logical_not(stays))
        def _():
            att_copy(0, head).start()
            lt_copy(0, a).start()
    for i in range(1, total):
        pa, pt = coords(i)
        att_copy(i, pt * ways + pa).wait_recv()
    for i in range(1, tp):
        pa, pt = coords(i)
        pltpu.make_async_remote_copy(
            src_ref=conv_ref.at[t], dst_ref=co_ref.at[pt],
            send_sem=csend.at[i], recv_sem=crecv.at[pt],
            device_id={"sp": me, "tp": pt}, device_id_type=MESH).wait_recv()
    for i in range(1, ways):
        lt_copy(i, lax.rem(a + i, ways)).wait_recv()
    for c in sends:
        c.wait_send()
    keep.wait()

    @pl.when(stays)
    def _():
        for c in mine:
            c.wait()

    if both:
        @pl.when(jnp.logical_not(stays))
        def _():
            att_copy(0, head).wait()
            lt_copy(0, a).wait()


def collect(att, lt, conv, ways, group, tp):
    any_ = pl.BlockSpec(memory_space=pl.ANY)
    rows, vdim = att.shape[2:]
    total = ways * tp
    return pl.pallas_call(
        lambda *refs: collect_kernel(ways, group, tp, *refs),
        out_shape=(
            jax.ShapeDtypeStruct((total, rows, vdim), att.dtype),
            jax.ShapeDtypeStruct(lt.shape, lt.dtype),
            jax.ShapeDtypeStruct(conv.shape, conv.dtype),
        ),
        in_specs=[any_] * 3,
        out_specs=(any_,) * 3,
        scratch_shapes=[
            pltpu.SemaphoreType.DMA((total,)),
            pltpu.SemaphoreType.DMA((total,)),
            pltpu.SemaphoreType.DMA((ways,)),
            pltpu.SemaphoreType.DMA((ways,)),
            pltpu.SemaphoreType.DMA((tp,)),
            pltpu.SemaphoreType.DMA((tp,)),
            pltpu.SemaphoreType.DMA((3,)),
        ],
        compiler_params=pltpu.CompilerParams(collective_id=2, has_side_effects=True),
        name="collect",
    )(att, lt, conv)


def attention(place, lam, head_gain, qt, kv, tile=512):
    ways, qdim, rows = qt.shape
    hd = qdim // 2
    blocks = kv.shape[0]
    vdim = head_gain.shape[0]
    group = blocks // ways
    tile = math.gcd(tile, rows)
    tiles = rows // tile
    def kernel(place_ref, lam_ref, gain_ref, q_ref, kv_ref, o_ref, lt_ref, sa, sb, acc_ref):
        i = pl.program_id(0); s = pl.program_id(1)
        chunk = i * group + flipped(place_ref[0], i, group)
        qs = [q_ref[0, m * hd:(m + 1) * hd, :] for m in range(2)]
        def score(j, ref):
            for m in range(2):
                ref[m] = jnp.dot(kv_ref[j, :rows, m * hd:(m + 1) * hd], qs[m], preferred_element_type=jnp.float32)
        def absorb(j, ref, tops, masked=False):
            vb = jnp.concatenate([kv_ref[j, rows + b * vdim:rows + (b + 1) * vdim] for b in range(rows // 128)], axis=1)
            vb = jnp.concatenate([vb, jnp.ones((16, rows), jnp.bfloat16)], axis=0)
            out=[]
            for m in range(2):
                sc = ref[m]
                if masked:
                    kp = lax.broadcasted_iota(jnp.int32, sc.shape, 0)
                    qp = lax.broadcasted_iota(jnp.int32, sc.shape, 1) + s * tile
                    sc = jnp.where(kp <= qp, sc, NEG)
                new = jnp.maximum(tops[m], jnp.max(sc, axis=0, keepdims=True))
                p = jnp.exp(sc - new)
                f = jnp.exp(tops[m] - new)
                acc_ref[m] = acc_ref[m] * f + jnp.dot(vb, p.astype(jnp.bfloat16), preferred_element_type=jnp.float32)
                out.append(new)
            return tuple(out)
        acc_ref[...] = jnp.zeros_like(acc_ref)
        one = jnp.full((1, tile), NEG, jnp.float32)
        score(chunk, sa)
        score(0, sb)
        tops = absorb(chunk, sa, (one, one), True)

        def pair(j, tops):
            score(2 * j + 1, sa)
            tops = absorb(2 * j, sb, tops)
            score(2 * j + 2, sb)
            return absorb(2 * j + 1, sa, tops)

        tops = lax.fori_loop(0, chunk // 2, pair, tops)
        tops = lax.cond(chunk % 2 == 1, lambda t: absorb(chunk - 1, sb, t), lambda t: t, tops)
        a0=acc_ref[0]; a1=acc_ref[1]
        t0,t1=tops
        l0=a0[vdim:vdim+1]; l1=a1[vdim:vdim+1]; a0=a0[:vdim]; a1=a1[:vdim]
        heads = a0 / l0 - lam_ref[0] * a1 / l1
        heads = heads * lax.rsqrt(jnp.mean(heads * heads, axis=0, keepdims=True) + 1e-06) * gain_ref[...]
        o_ref[0] = heads.T.astype(jnp.bfloat16)
        lt_ref[0, 0:1, :] = t0 + jnp.log(l0)
        lt_ref[0, 1:2, :] = t1 + jnp.log(l1)
    smem = pl.BlockSpec(memory_space=pltpu.SMEM)
    return pl.pallas_call(kernel, grid=(ways, tiles),
        out_shape=(jax.ShapeDtypeStruct((ways, rows, vdim), jnp.bfloat16), jax.ShapeDtypeStruct((ways, 2, rows), jnp.float32)),
        in_specs=[smem, smem, pl.BlockSpec((vdim, 1), lambda i, s: (0, 0)), pl.BlockSpec((1, qdim, tile), lambda i, s: (i, 0, s)), pl.BlockSpec(kv.shape, lambda i, s: (0, 0, 0))],
        out_specs=(pl.BlockSpec((1, tile, vdim), lambda i, s: (i, s, 0)), pl.BlockSpec((1, 2, tile), lambda i, s: (i, 0, s))),
        scratch_shapes=[pltpu.VMEM((2,rows,tile),jnp.float32),pltpu.VMEM((2,rows,tile),jnp.float32),pltpu.VMEM((2,vdim+16,tile),jnp.float32)],
        compiler_params=pltpu.CompilerParams(vmem_limit_bytes=58 << 20), name="attend")(place, lam, head_gain.reshape(-1, 1), qt, kv)


def prepare_t(raw, qk_gain, cosine, sine):
    values = raw.astype(jnp.float32)
    values = values * lax.rsqrt(jnp.mean(values * values, axis=2, keepdims=True) + 1e-06)
    values = values * qk_gain[None, :, :, None]
    half = raw.shape[2] // 2
    first, second = values[:, :, :half], values[:, :, half:]
    return jnp.concatenate(
        [first * cosine - second * sine, second * cosine + first * sine], axis=2
    ).astype(jnp.bfloat16)


def per_device(
    tokens, norm_gain, query_weight, key_weight, value_weight, glu_value_weight, glu_gate_weight,
    qk_gain, mix_lambda, head_gain, conv_kernel, channel_gain, channel_shift, output_weight,
):
    head_size = qk_gain.shape[1]
    heads_here = mix_lambda.shape[0]
    value_size = head_gain.shape[0]
    kernel_len = conv_kernel.shape[0]
    conv_here = conv_kernel.shape[1]
    width = tokens.shape[1]
    sp = lax.axis_size("sp")
    tp = lax.axis_size("tp")
    me = lax.axis_index("sp")
    t = lax.axis_index("tp")
    ways = heads_here
    group = sp // ways
    own = tokens.shape[0]
    rows = own * tp

    def norm(piece):
        inputs = piece.astype(jnp.float32)
        return (
            inputs * lax.rsqrt(jnp.mean(inputs * inputs, axis=-1, keepdims=True) + 1e-06) * norm_gain
        ).astype(jnp.bfloat16)

    others = [tokens] + [
        lax.ppermute(tokens, "tp", [(i, (i - d) % tp) for i in range(tp)]) for d in range(1, tp)
    ]
    if tp == 2:
        other = others[1]
        normed = norm(jnp.concatenate([jnp.where(t == 0, tokens, other), jnp.where(t == 0, other, tokens)], axis=0))
    else:
        stacked = jnp.stack(others)
        normed = norm(jnp.concatenate(
            [lax.dynamic_index_in_dim(stacked, (j - t) % tp, 0, keepdims=False) for j in range(tp)], axis=0))

    def turned(matrix):
        return lax.dot_general(matrix, normed, (((0,), (1,)), ((), ())), preferred_element_type=jnp.float32).astype(jnp.bfloat16)

    def plain(matrix):
        return jnp.dot(normed, matrix, preferred_element_type=jnp.float32).astype(jnp.bfloat16)

    positions = (me * rows + jnp.arange(rows, dtype=jnp.int32)).astype(jnp.float32)
    inverse = 10000.0 ** (-jnp.arange(0, head_size // 2, dtype=jnp.float32) * 2.0 / head_size)
    angles = positions[None, :] * inverse[:, None]
    cosine, sine = jnp.cos(angles)[None, None], jnp.sin(angles)[None, None]
    shape = (heads_here, 2, head_size, rows)
    rq = prepare_t(turned(query_weight).reshape(shape), qk_gain, cosine, sine) * jnp.bfloat16(head_size ** -0.5)
    rk = prepare_t(turned(key_weight).reshape(shape), qk_gain, cosine, sine)
    qt = rq.reshape(heads_here, 2 * head_size, rows)
    kk = jnp.transpose(rk.reshape(heads_here, 2 * head_size, rows), (0, 2, 1))
    vt = turned(value_weight).reshape(heads_here, value_size, rows)
    kv = jnp.concatenate([kk, vt.reshape(heads_here, value_size, rows // 128, 128).transpose(0, 2, 1, 3).reshape(heads_here, -1, 128)], axis=1)
    qall, kvall = spread(qt, kv, ways, group)

    glu_a, glu_g = plain(glu_value_weight), plain(glu_gate_weight)
    gated = (glu_a.astype(jnp.float32) * jax.nn.sigmoid(glu_g.astype(jnp.float32))).astype(jnp.bfloat16)
    earlier = from_behind(gated[rows - (kernel_len - 1):], "sp", 1)
    extended = jnp.concatenate([earlier, gated], axis=0).astype(jnp.float32)
    convolved = jnp.zeros((rows, conv_here), jnp.float32)
    for step in range(kernel_len):
        convolved = convolved + conv_kernel[step][None, :] * extended[step:step + rows]
    plain_sum, square_sum = lax.psum(
        (jnp.sum(convolved, axis=1), jnp.sum(convolved * convolved, axis=1)), "tp"
    )
    channels = conv_here * tp
    middle = (plain_sum / channels)[:, None]
    spread_ = (square_sum / channels)[:, None] - middle * middle
    conv_out = jax.nn.silu(
        (convolved - middle) * lax.rsqrt(spread_ + 1e-05) * channel_gain + channel_shift
    ).astype(jnp.bfloat16)

    place = (me % group).astype(jnp.int32).reshape(1)
    lam = lax.dynamic_slice(mix_lambda, (me // group,), (1,))
    att, lt = attention(place, lam, head_gain, qall, kvall)
    ao, lo, co = collect(
        att.reshape(ways, tp, own, value_size), lt, conv_out.reshape(tp, own, conv_here), ways, group, tp)
    heads = ways * tp
    merged = jnp.concatenate([
        jnp.transpose(ao, (1, 0, 2)).reshape(own, heads * value_size),
        jnp.transpose(co, (1, 0, 2)).reshape(own, channels)], axis=1)
    mixed = jnp.dot(merged, output_weight, preferred_element_type=jnp.float32).astype(jnp.bfloat16)
    return (mixed, jnp.transpose(lo, (1, 0, 2)))


def solution(mesh):
    placed = (
        P(("sp", "tp"), None), P(), P(None, "tp"), P(None, "tp"), P(None, "tp"), P(None, "tp"), P(None, "tp"),
        P(), P("tp"), P(), P(None, "tp"), P("tp"), P("tp"), P(),
    )
    return jax.shard_map(
        per_device,
        mesh=mesh,
        in_specs=placed,
        out_specs=(P(("sp", "tp"), None), P(None, "tp", "sp")),
        check_vma=False,
    )
```

```python
import math

import jax
import jax.numpy as jnp
from jax import lax
from jax.experimental import pallas as pl
from jax.experimental.pallas import tpu as pltpu
from jax.sharding import PartitionSpec as P

MESH = pl.DeviceIdType.MESH
NEG = -1e30


def from_behind(value, axis, steps):
    count = lax.axis_size(axis)
    leading, last = (max(0, -steps), min(count, count - steps))
    return lax.ppermute(value, axis, [(source, source + steps) for source in range(leading, last)])


def flipped(g, a, group):
    if group % 2:
        return g
    return jnp.where(a % 2 == 0, g, group - 1 - g)


def spread_kernel(ways, group, q_ref, kv_ref, qo_ref, kvo_ref, qsend, qrecv, ksend, kfwd, krelay, krecv, local):
    me = lax.axis_index("sp")
    a = me // group
    g = me % group
    cores = 2 if group % 2 == 0 else 1
    half = group // cores
    mate = a * group + (g + 1 - 2 * (g % 2)) if cores == 2 else me

    def same(d):
        return (g + d * cores) % group

    peers = [lax.rem(a + d, ways) * group + g for d in range(1, ways)]
    peers += [a * group + same(d) for d in range(1, half)]
    if cores == 2:
        peers.append(mate)
        peers += [lax.rem(a + d, ways) * group + group - 1 - g for d in range(ways)]
    barrier = pltpu.get_barrier_semaphore()
    for peer in peers:
        pl.semaphore_signal(barrier, inc=1, device_id={"sp": peer}, device_id_type=MESH)
    pl.semaphore_wait(barrier, len(peers))

    def kv_copy(src, slot, send, peer):
        return pltpu.make_async_remote_copy(
            src_ref=src, dst_ref=kvo_ref.at[slot], send_sem=send, recv_sem=krecv.at[slot],
            device_id={"sp": peer}, device_id_type=MESH)

    sends = []
    keep = pltpu.make_async_copy(kv_ref.at[a], kvo_ref.at[me], local.at[0])
    keep_q = pltpu.make_async_copy(q_ref.at[a], qo_ref.at[a], local.at[1])
    keep.start()

    def q_copy(h, slot, d):
        return pltpu.make_async_remote_copy(
            src_ref=q_ref.at[h], dst_ref=qo_ref.at[slot], send_sem=qsend.at[d], recv_sem=qrecv.at[slot],
            device_id={"sp": h * group + flipped(g, a, group)}, device_id_type=MESH)

    stays = a % 2 == 0 if cores == 2 else a >= 0

    @pl.when(stays)
    def _():
        keep_q.start()
    order = list(range(1, ways))
    for d in order:
        h = lax.rem(a + d, ways)
        c = kv_copy(kv_ref.at[h], me, ksend.at[d - 1], h * group + g)
        c.start()
        sends.append(c)

    def forward(d):
        src_a = lax.rem(a + ways - d, ways)
        slot = src_a * group + g
        if d:
            kv_copy(kvo_ref.at[slot], slot, ksend.at[d - 1], me).wait_recv()
            src = kvo_ref.at[slot]
        else:
            src = kv_ref.at[a]
        n = 0
        for e in range(1, half):
            c = kv_copy(src, slot, kfwd.at[d, n], a * group + same(e))
            c.start()
            sends.append(c)
            n += 1
        if cores == 2:
            c = kv_copy(src, slot, kfwd.at[d, n], mate)
            c.start()
            sends.append(c)

    def relay(d):
        src_a = lax.rem(a + ways - d, ways)
        for e in range(1, half):
            slot = src_a * group + same(e)
            kv_copy(kvo_ref.at[slot], slot, krelay.at[d, e - 1], mate).wait_recv()
            if cores == 2:
                c = kv_copy(kvo_ref.at[slot], slot, krelay.at[d, e - 1], mate)
                c.start()
                sends.append(c)

    forward(0)
    for d in order:
        c = q_copy(lax.rem(a + d, ways), a, d)
        c.start()
        sends.append(c)
    if cores == 2:
        @pl.when(jnp.logical_not(stays))
        def _():
            q_copy(a, a, 0).start()
    for d in range(1, ways):
        forward(d)
        relay(d - 1)
    relay(ways - 1)
    if cores == 2:
        for d in range(ways):
            src_a = lax.rem(a + ways - d, ways)
            for e in range(half):
                slot = src_a * group + (g + 1 - 2 * (g % 2) + e * cores) % group
                kv_copy(kvo_ref.at[slot], slot, krelay.at[0, 0], mate).wait_recv()
    for d in range(1, ways):
        src_a = lax.rem(a + ways - d, ways)
        q_copy(a, src_a, d).wait_recv()
    for c in sends:
        c.wait_send()
    keep.wait()

    @pl.when(stays)
    def _():
        keep_q.wait()

    if cores == 2:
        @pl.when(jnp.logical_not(stays))
        def _():
            q_copy(a, a, 0).wait()


def spread(q, kv, ways, group):
    cores = 2 if group % 2 == 0 else 1
    half = group // cores
    any_ = pl.BlockSpec(memory_space=pl.ANY)
    n = max(ways - 1, 1)
    return pl.pallas_call(
        lambda *refs: spread_kernel(ways, group, *refs),
        out_shape=(
            jax.ShapeDtypeStruct(q.shape, q.dtype),
            jax.ShapeDtypeStruct((ways * group,) + kv.shape[1:], kv.dtype),
        ),
        in_specs=[any_, any_],
        out_specs=(any_, any_),
        scratch_shapes=[
            pltpu.SemaphoreType.DMA((ways,)),
            pltpu.SemaphoreType.DMA((ways,)),
            pltpu.SemaphoreType.DMA((n,)),
            pltpu.SemaphoreType.DMA((ways, half)),
            pltpu.SemaphoreType.DMA((ways, max(half - 1, 1))),
            pltpu.SemaphoreType.DMA((ways * group,)),
            pltpu.SemaphoreType.DMA((2,)),
        ],
        compiler_params=pltpu.CompilerParams(collective_id=1, has_side_effects=True),
        name="spread",
    )(q, kv)


def collect_kernel(ways, group, tp, att_ref, lt_ref, ao_ref, lo_ref, asend, arecv, lsend, lrecv, local):
    me = lax.axis_index("sp")
    t = lax.axis_index("tp")
    a = me // group
    g = me % group
    vdim = att_ref.shape[-1]

    def coords(i):
        dt, da = i % tp, i // tp
        return lax.rem(a + da, ways), lax.rem(t + dt, tp)

    total = ways * tp
    both = group % 2 == 0
    barrier = pltpu.get_barrier_semaphore()
    for i in range(total):
        pa, pt = coords(i)
        if i:
            pl.semaphore_signal(barrier, inc=1, device_id={"sp": pa * group + g, "tp": pt}, device_id_type=MESH)
        if both:
            pl.semaphore_signal(
                barrier, inc=1, device_id={"sp": pa * group + group - 1 - g, "tp": pt}, device_id_type=MESH)
    pl.semaphore_wait(barrier, 2 * total - 1 if both else total - 1)

    head = t * ways + a

    def lanes(slot):
        return ao_ref.at[:, pl.ds(pl.multiple_of(slot * vdim, 128), vdim)]

    def att_copy(i, slot):
        pa, pt = coords(i)
        return pltpu.make_async_remote_copy(
            src_ref=att_ref.at[pa, pt], dst_ref=lanes(slot), send_sem=asend.at[i], recv_sem=arecv.at[slot],
            device_id={"sp": pa * group + flipped(g, pa, group), "tp": pt}, device_id_type=MESH)

    def lt_copy(i, slot):
        pa = lax.rem(a + i, ways)
        return pltpu.make_async_remote_copy(
            src_ref=lt_ref.at[pa], dst_ref=lo_ref.at[slot], send_sem=lsend.at[i], recv_sem=lrecv.at[slot],
            device_id={"sp": pa * group + flipped(g, pa, group), "tp": t}, device_id_type=MESH)

    stays = a % 2 == 0 if both else a >= 0
    sends = []
    for i in range(total - 1, 0, -1):
        c = att_copy(i, head)
        c.start()
        sends.append(c)
    for i in range(1, ways):
        c = lt_copy(i, a)
        c.start()
        sends.append(c)
    mine = [
        pltpu.make_async_copy(att_ref.at[a, t], lanes(head), local.at[0]),
        pltpu.make_async_copy(lt_ref.at[a], lo_ref.at[a], local.at[2]),
    ]

    @pl.when(stays)
    def _():
        for c in mine:
            c.start()

    if both:
        @pl.when(jnp.logical_not(stays))
        def _():
            att_copy(0, head).start()
            lt_copy(0, a).start()
    for i in range(1, total):
        pa, pt = coords(i)
        att_copy(i, pt * ways + pa).wait_recv()
    for i in range(1, ways):
        lt_copy(i, lax.rem(a + i, ways)).wait_recv()
    for c in sends:
        c.wait_send()

    @pl.when(stays)
    def _():
        for c in mine:
            c.wait()

    if both:
        @pl.when(jnp.logical_not(stays))
        def _():
            att_copy(0, head).wait()
            lt_copy(0, a).wait()


def collect(att, lt, ways, group, tp):
    any_ = pl.BlockSpec(memory_space=pl.ANY)
    rows, vdim = att.shape[2:]
    total = ways * tp
    return pl.pallas_call(
        lambda *refs: collect_kernel(ways, group, tp, *refs),
        out_shape=(
            jax.ShapeDtypeStruct((rows, total * vdim), att.dtype),
            jax.ShapeDtypeStruct(lt.shape, lt.dtype),
        ),
        in_specs=[any_] * 2,
        out_specs=(any_,) * 2,
        scratch_shapes=[
            pltpu.SemaphoreType.DMA((total,)),
            pltpu.SemaphoreType.DMA((total,)),
            pltpu.SemaphoreType.DMA((ways,)),
            pltpu.SemaphoreType.DMA((ways,)),
            pltpu.SemaphoreType.DMA((3,)),
        ],
        compiler_params=pltpu.CompilerParams(collective_id=2, has_side_effects=True),
        cost_estimate=pl.CostEstimate(flops=0, bytes_accessed=32 * att.size, transcendentals=0),
        name="collect",
    )(att, lt)


def attention(place, lam, head_gain, qt, kv, tile=512):
    ways, qdim, rows = qt.shape
    hd = qdim // 2
    blocks = kv.shape[0]
    vdim = head_gain.shape[0]
    group = blocks // ways
    tile = math.gcd(tile, rows)
    tiles = rows // tile
    def kernel(place_ref, lam_ref, gain_ref, q_ref, kv_ref, o_ref, lt_ref, sa, sb, acc_ref):
        i = pl.program_id(0); s = pl.program_id(1)
        chunk = i * group + flipped(place_ref[0], i, group)
        qs = [q_ref[0, m * hd:(m + 1) * hd, :] for m in range(2)]
        def score(j, ref):
            for m in range(2):
                ref[m] = jnp.dot(kv_ref[j, :rows, m * hd:(m + 1) * hd], qs[m], preferred_element_type=jnp.float32)
        def absorb(j, ref, tops, masked=False):
            vb = jnp.concatenate([kv_ref[j, rows + b * vdim:rows + (b + 1) * vdim] for b in range(rows // 128)], axis=1)
            vb = jnp.concatenate([vb, jnp.ones((16, rows), jnp.bfloat16)], axis=0)
            out=[]
            for m in range(2):
                sc = ref[m]
                if masked:
                    kp = lax.broadcasted_iota(jnp.int32, sc.shape, 0)
                    qp = lax.broadcasted_iota(jnp.int32, sc.shape, 1) + s * tile
                    sc = jnp.where(kp <= qp, sc, NEG)
                new = jnp.maximum(tops[m], jnp.max(sc, axis=0, keepdims=True))
                p = jnp.exp(sc - new)
                f = jnp.exp(tops[m] - new)
                acc_ref[m] = acc_ref[m] * f + jnp.dot(vb, p.astype(jnp.bfloat16), preferred_element_type=jnp.float32)
                out.append(new)
            return tuple(out)
        acc_ref[...] = jnp.zeros_like(acc_ref)
        one = jnp.full((1, tile), NEG, jnp.float32)
        score(chunk, sa)
        score(0, sb)
        tops = absorb(chunk, sa, (one, one), True)

        def pair(j, tops):
            score(2 * j + 1, sa)
            tops = absorb(2 * j, sb, tops)
            score(2 * j + 2, sb)
            return absorb(2 * j + 1, sa, tops)

        tops = lax.fori_loop(0, chunk // 2, pair, tops)
        tops = lax.cond(chunk % 2 == 1, lambda t: absorb(chunk - 1, sb, t), lambda t: t, tops)
        a0=acc_ref[0]; a1=acc_ref[1]
        t0,t1=tops
        l0=a0[vdim:vdim+1]; l1=a1[vdim:vdim+1]; a0=a0[:vdim]; a1=a1[:vdim]
        heads = a0 / l0 - lam_ref[0] * a1 / l1
        heads = heads * lax.rsqrt(jnp.mean(heads * heads, axis=0, keepdims=True) + 1e-06) * gain_ref[...]
        o_ref[0] = heads.T.astype(jnp.bfloat16)
        lt_ref[0, 0:1, :] = t0 + jnp.log(l0)
        lt_ref[0, 1:2, :] = t1 + jnp.log(l1)
    smem = pl.BlockSpec(memory_space=pltpu.SMEM)
    return pl.pallas_call(kernel, grid=(ways, tiles),
        out_shape=(jax.ShapeDtypeStruct((ways, rows, vdim), jnp.bfloat16), jax.ShapeDtypeStruct((ways, 2, rows), jnp.float32)),
        in_specs=[smem, smem, pl.BlockSpec((vdim, 1), lambda i, s: (0, 0)), pl.BlockSpec((1, qdim, tile), lambda i, s: (i, 0, s)), pl.BlockSpec(kv.shape, lambda i, s: (0, 0, 0))],
        out_specs=(pl.BlockSpec((1, tile, vdim), lambda i, s: (i, s, 0)), pl.BlockSpec((1, 2, tile), lambda i, s: (i, 0, s))),
        scratch_shapes=[pltpu.VMEM((2,rows,tile),jnp.float32),pltpu.VMEM((2,rows,tile),jnp.float32),pltpu.VMEM((2,vdim+16,tile),jnp.float32)],
        compiler_params=pltpu.CompilerParams(vmem_limit_bytes=40 << 20), name="attend",
        cost_estimate=pl.CostEstimate(
            flops=blocks * rows * ways * rows * 6 * vdim, bytes_accessed=2 * kv.size,
            transcendentals=blocks * rows * ways * rows))(place, lam, head_gain.reshape(-1, 1), qt, kv)


def prepare_t(raw, qk_gain, cosine, sine):
    values = raw.astype(jnp.float32)
    values = values * lax.rsqrt(jnp.mean(values * values, axis=2, keepdims=True) + 1e-06)
    values = values * qk_gain[None, :, :, None]
    half = raw.shape[2] // 2
    first, second = values[:, :, :half], values[:, :, half:]
    return jnp.concatenate(
        [first * cosine - second * sine, second * cosine + first * sine], axis=2
    ).astype(jnp.bfloat16)


def per_device(
    tokens, norm_gain, query_weight, key_weight, value_weight, glu_value_weight, glu_gate_weight,
    qk_gain, mix_lambda, head_gain, conv_kernel, channel_gain, channel_shift, output_weight,
):
    head_size = qk_gain.shape[1]
    heads_here = mix_lambda.shape[0]
    value_size = head_gain.shape[0]
    kernel_len = conv_kernel.shape[0]
    conv_here = conv_kernel.shape[1]
    width = tokens.shape[1]
    sp = lax.axis_size("sp")
    tp = lax.axis_size("tp")
    me = lax.axis_index("sp")
    t = lax.axis_index("tp")
    ways = heads_here
    group = sp // ways
    own = tokens.shape[0]
    rows = own * tp

    def norm(piece):
        inputs = piece.astype(jnp.float32)
        return (
            inputs * lax.rsqrt(jnp.mean(inputs * inputs, axis=-1, keepdims=True) + 1e-06) * norm_gain
        ).astype(jnp.bfloat16)

    others = [tokens] + [
        lax.ppermute(tokens, "tp", [(i, (i - d) % tp) for i in range(tp)]) for d in range(1, tp)
    ]
    if tp == 2:
        other = others[1]
        normed = norm(jnp.concatenate([jnp.where(t == 0, tokens, other), jnp.where(t == 0, other, tokens)], axis=0))
    else:
        stacked = jnp.stack(others)
        normed = norm(jnp.concatenate(
            [lax.dynamic_index_in_dim(stacked, (j - t) % tp, 0, keepdims=False) for j in range(tp)], axis=0))

    def turned(matrix):
        return lax.dot_general(matrix, normed, (((0,), (1,)), ((), ())), preferred_element_type=jnp.float32).astype(jnp.bfloat16)

    def plain(matrix):
        return jnp.dot(normed, matrix, preferred_element_type=jnp.float32).astype(jnp.bfloat16)

    positions = (me * rows + jnp.arange(rows, dtype=jnp.int32)).astype(jnp.float32)
    inverse = 10000.0 ** (-jnp.arange(0, head_size // 2, dtype=jnp.float32) * 2.0 / head_size)
    angles = positions[None, :] * inverse[:, None]
    cosine, sine = jnp.cos(angles)[None, None], jnp.sin(angles)[None, None]
    shape = (heads_here, 2, head_size, rows)
    rq = prepare_t(turned(query_weight).reshape(shape), qk_gain, cosine, sine) * jnp.bfloat16(head_size ** -0.5)
    rk = prepare_t(turned(key_weight).reshape(shape), qk_gain, cosine, sine)
    qt = rq.reshape(heads_here, 2 * head_size, rows)
    kk = jnp.transpose(rk.reshape(heads_here, 2 * head_size, rows), (0, 2, 1))
    vt = turned(value_weight).reshape(heads_here, value_size, rows)
    kv = jnp.concatenate([kk, vt.reshape(heads_here, value_size, rows // 128, 128).transpose(0, 2, 1, 3).reshape(heads_here, -1, 128)], axis=1)
    qall, kvall = spread(qt, kv, ways, group)

    glu_a, glu_g = plain(glu_value_weight), plain(glu_gate_weight)
    gated = (glu_a.astype(jnp.float32) * jax.nn.sigmoid(glu_g.astype(jnp.float32))).astype(jnp.bfloat16)
    earlier = from_behind(gated[rows - (kernel_len - 1):], "sp", 1)
    extended = jnp.concatenate([earlier, gated], axis=0).astype(jnp.float32)
    convolved = jnp.zeros((rows, conv_here), jnp.float32)
    for step in range(kernel_len):
        convolved = convolved + conv_kernel[step][None, :] * extended[step:step + rows]
    plain_sum, square_sum = lax.psum(
        (jnp.sum(convolved, axis=1), jnp.sum(convolved * convolved, axis=1)), "tp"
    )
    channels = conv_here * tp
    middle = (plain_sum / channels)[:, None]
    spread_ = (square_sum / channels)[:, None] - middle * middle
    conv_out = jax.nn.silu(
        (convolved - middle) * lax.rsqrt(spread_ + 1e-05) * channel_gain + channel_shift
    ).astype(jnp.bfloat16)

    place = (me % group).astype(jnp.int32).reshape(1)
    lam = lax.dynamic_slice(mix_lambda, (me // group,), (1,))
    att, lt = attention(place, lam, head_gain, qall, kvall)
    pieces = conv_out.reshape(tp, own, conv_here)
    got = [lax.dynamic_index_in_dim(pieces, t, 0, keepdims=False)]
    for d in range(1, tp):
        piece = lax.dynamic_index_in_dim(pieces, (t + d) % tp, 0, keepdims=False)
        got.append(lax.ppermute(piece, "tp", [(i, (i + d) % tp) for i in range(tp)]))
    if tp == 2:
        first = jnp.where(t == 0, got[0], got[1])
        second = jnp.where(t == 0, got[1], got[0])
        co = [first, second]
    else:
        stack = jnp.stack(got)
        co = [lax.dynamic_index_in_dim(stack, (t - j) % tp, 0, keepdims=False) for j in range(tp)]
    ao, lo = collect(att.reshape(ways, tp, own, value_size), lt, ways, group, tp)
    merged = jnp.concatenate([ao] + co, axis=1)
    mixed = jnp.dot(merged, output_weight, preferred_element_type=jnp.float32).astype(jnp.bfloat16)
    return (mixed, jnp.transpose(lo, (1, 0, 2)))


def solution(mesh):
    placed = (
        P(("sp", "tp"), None), P(), P(None, "tp"), P(None, "tp"), P(None, "tp"), P(None, "tp"), P(None, "tp"),
        P(), P("tp"), P(), P(None, "tp"), P("tp"), P("tp"), P(),
    )
    return jax.shard_map(
        per_device,
        mesh=mesh,
        in_specs=placed,
        out_specs=(P(("sp", "tp"), None), P(None, "tp", "sp")),
        check_vma=False,
    )
```
